32 devices in a mesh: sp: 8 (over z, x), tp: 4 (over y, core).
Axes of the slice: x: 2, y: 2, z: 4, core: 2. Of those that a mesh axis runs over, the one named last changes fastest.
Arguments:
- tokens: bfloat16 [8192, 4096], P('sp'), may hold values from -6 to 6
- input_norm_scale: bfloat16 [4096], replicated, may hold values from 0.099609375 to 1.8984375
- mean_input_weight: bfloat16 [4096, 2048], P('sp', 'tp'), may hold values from -0.09375 to 0.09375
- query_matrix: bfloat16 [4096, 2048], P('sp', 'tp'), may hold values from -0.09375 to 0.09375
- key_matrix: bfloat16 [4096, 2048], P('sp', 'tp'), may hold values from -0.09375 to 0.09375
- value_matrix: bfloat16 [4096, 2048], P('sp', 'tp'), may hold values from -0.09375 to 0.09375
- strength_weight: bfloat16 [4096, 16], P('sp', 'tp'), may hold values from -0.09375 to 0.09375
- decay_input_weight: bfloat16 [4096, 16], P('sp', 'tp'), may hold values from -0.25 to 0.25
- causal_filter_weight: bfloat16 [4, 3, 2048], replicated, may hold values from -3 to 3
- head_decay_logrates: float32 [16], replicated, may hold values from -13.2 to -2.9
- decay_input_shift: float32 [16], replicated, may hold values from -1 to 1
- strength_shift: float32 [16], replicated, may hold values from -5 to -3
- decay_spike: float32 [8192, 16], P('sp', 'tp'), may hold values from -1.3 to 0
- head_norm_scale: bfloat16 [128], replicated, may hold values from 0.099609375 to 1.8984375
- group_mixing_weight: bfloat16 [16, 128, 128], replicated, may hold values from -0.5 to 0.5
- mean_channel_scale: bfloat16 [2048], replicated, may hold values from 0.099609375 to 1.8984375
- mean_output_weight: bfloat16 [2048, 4096], P('tp', 'sp'), may hold values from -0.09375 to 0.09375
- delta_output_weight: bfloat16 [2048, 4096], P('tp', 'sp'), may hold values from -0.09375 to 0.09375
Outputs:
- mixed_out: bfloat16 [8192, 4096], P(('sp', 'tp'))
The draws below stay inside these ranges and needn't reach their ends.
All inputs are finite; a program needn't handle non-finite values.
Results may differ from the reference program's by a relative error of at most 0.015.
Values may be sent and summed in bfloat16 or wider, within the bound.
A program may use at most 128 MiB of HBM per device.

```python
import jax
import jax.numpy as jnp
from jax import lax

D = 4096
POOL_GROUPS = 16
GROUP_DIM = 128
MIXER_HEADS = 16
HEAD_DIM = 128
CONV = 4
BLOCK = 64
TOK_DEV = 1024
POOL_W = 2048
GDN_W = 2048
SEQUENCE_TOKENS = 8192
N_TP = 4


def draw_head_decay_logrates(key, part):
    ranking = jax.random.permutation(jax.random.fold_in(key, 11), MIXER_HEADS)
    fast_count = MIXER_HEADS // 2
    fast_rate = jax.random.uniform(jax.random.fold_in(key, 12), (MIXER_HEADS,), jnp.float32, jnp.log(0.012), jnp.log(0.035))
    slow_rate = jax.random.uniform(jax.random.fold_in(key, 13), (MIXER_HEADS,), jnp.float32, jnp.log(2e-06), jnp.log(2e-05))
    return jnp.where(ranking < fast_count, fast_rate, slow_rate).astype(jnp.float32)


def draw_decay_spike(key, part):
    block_ids = jnp.arange(SEQUENCE_TOKENS) // TOK_DEV
    block_rates = jnp.exp(jax.random.uniform(jax.random.fold_in(key, 21), (SEQUENCE_TOKENS // TOK_DEV, MIXER_HEADS), jnp.float32, jnp.log(1e-06), jnp.log(2e-05)))
    stable_portion = -block_rates[block_ids]
    spike_rows = jax.random.randint(jax.random.fold_in(key, 22), (2, MIXER_HEADS), 0, SEQUENCE_TOKENS)
    error_values = jax.random.uniform(jax.random.fold_in(key, 23), (2, MIXER_HEADS), jnp.float32, 0.2, 0.45)
    match_flags = jnp.arange(SEQUENCE_TOKENS)[:, None, None] == spike_rows[None, :, :]
    spike_portion = jnp.sum(jnp.where(match_flags, jnp.log(1.0 - error_values)[None, :, :], 0.0), axis=1)
    return (stable_portion + spike_portion).astype(jnp.float32)


def block_levels(stream_key, dims, split, smallest, largest):
    factor_of, own = 1.0, jax.random.fold_in(stream_key, 6)
    for dim, shards_of in split:
        heights = jnp.exp(jax.random.uniform(jax.random.fold_in(own, dim), (shards_of,), jnp.float32, smallest / len(split), largest / len(split)))
        factor_of = factor_of * jnp.repeat(heights, dims[dim] // shards_of).reshape([-1 if axis == dim else 1 for axis in range(len(dims))])
    return factor_of


def bell_draw(own_key, shape, scale, reach, split=(), held_as=jnp.bfloat16):
    drawn = jax.random.normal(own_key, shape, jnp.float32) * scale
    if len(split) > 0:
        drawn = block_levels(own_key, shape, split, -0.22, 0.18) * drawn
    return jnp.clip(drawn, min=-reach, max=reach).astype(held_as)


def setup_inputs(seed: int = 0) -> dict:
    seeds = jax.random.split(jax.random.key(seed), 19)
    return {
        "tokens": bell_draw(seeds[0], (SEQUENCE_TOKENS, D), 1.0, 6.0, ((0, 8),)),
        "input_norm_scale": jnp.clip(1.0 + 0.18 * jax.random.normal(seeds[1], (D,), jnp.float32), 0.099609375, 1.8984375).astype(jnp.bfloat16),
        "mean_input_weight": bell_draw(seeds[2], (D, POOL_W), D ** -0.5, 0.09375, ((0, 8), (1, 4))),
        "query_matrix": bell_draw(seeds[3], (D, GDN_W), D ** -0.5, 0.09375, ((0, 8), (1, 4))),
        "key_matrix": bell_draw(seeds[4], (D, GDN_W), D ** -0.5, 0.09375, ((0, 8), (1, 4))),
        "value_matrix": bell_draw(seeds[5], (D, GDN_W), D ** -0.5, 0.09375, ((0, 8), (1, 4))),
        "strength_weight": bell_draw(seeds[6], (D, MIXER_HEADS), D ** -0.5, 0.09375, ((0, 8), (1, 4))),
        "decay_input_weight": bell_draw(seeds[7], (D, MIXER_HEADS), (D // 9) ** -0.5, 0.25, ((0, 8), (1, 4))),
        "causal_filter_weight": bell_draw(seeds[8], (CONV, 3, GDN_W), CONV ** -0.5, 3.0),
        "head_decay_logrates": draw_head_decay_logrates(jax.random.fold_in(seeds[18], 71), 0),
        "decay_input_shift": jnp.clip(jax.random.uniform(seeds[10], (MIXER_HEADS,), jnp.float32, -1.0, 1.0), -1.0, 1.0),
        "strength_shift": jnp.clip(jax.random.uniform(seeds[11], (MIXER_HEADS,), jnp.float32, -5.0, -3.0), -5.0, -3.0),
        "decay_spike": draw_decay_spike(jax.random.fold_in(seeds[18], 71), 0),
        "head_norm_scale": jnp.clip(1.0 + 0.18 * jax.random.normal(seeds[13], (HEAD_DIM,), jnp.float32), 0.099609375, 1.8984375).astype(jnp.bfloat16),
        "group_mixing_weight": bell_draw(seeds[14], (POOL_GROUPS, GROUP_DIM, GROUP_DIM), GROUP_DIM ** -0.5, 0.5),
        "mean_channel_scale": jnp.clip(1.0 + 0.18 * jax.random.normal(seeds[15], (POOL_W,), jnp.float32), 0.099609375, 1.8984375).astype(jnp.bfloat16),
        "mean_output_weight": bell_draw(seeds[16], (POOL_W, D), (POOL_W + GDN_W) ** -0.5, 0.09375, ((0, 4), (1, 8))),
        "delta_output_weight": bell_draw(seeds[17], (GDN_W, D), (POOL_W + GDN_W) ** -0.5, 0.09375, ((0, 4), (1, 8))),
    }


EPSILON = 1e-06

def scale_rows(values, gain_vec):
    squares = lax.optimization_barrier(jnp.mean(values * values, axis=-1, keepdims=True))
    return values * lax.rsqrt(squares + EPSILON) * gain_vec.astype(jnp.float32)

def unit_rows(values):
    return values * lax.rsqrt(lax.optimization_barrier(jnp.sum(values * values, axis=-1, keepdims=True)) + EPSILON)

def causal_taps(extended, taps, rows_out):
    tap_sum = jnp.zeros((rows_out, taps.shape[1]), jnp.float32)
    for tap_index in range(taps.shape[0]):
        tap_sum = tap_sum + taps[tap_index] * extended[tap_index:tap_index + rows_out]
    return jax.nn.silu(tap_sum)

def pool_means(previous, current, group_ids, positions):
    pool_reach = 15
    rows_out = current.shape[0]
    extended = jnp.concatenate([previous, current], axis=0).astype(jnp.float32)
    window_size = jnp.left_shift(jnp.int32(2), (group_ids % 4).astype(jnp.int32))
    windowed = jnp.zeros(current.shape, jnp.float32)
    for lag_rows in range(pool_reach + 1):
        shifted = extended[pool_reach - lag_rows:pool_reach - lag_rows + rows_out]
        windowed = windowed + jnp.where(lag_rows < window_size[None, :], shifted, 0.0)
    counts = jnp.minimum(positions[:, None] + 1, window_size[None, :]).astype(jnp.float32)
    return (windowed / counts - extended[pool_reach:]).astype(jnp.bfloat16)

def block_terms(query, keys, values, decay_logarithm, beta):
    blocks = keys.shape[0] // BLOCK

    def to_blocks(tensor):
        return jnp.swapaxes(tensor.reshape((blocks, BLOCK) + tensor.shape[1:]), 1, 2)
    query_b = to_blocks(query)
    keys_b = to_blocks(keys)
    values_b = to_blocks(values)
    decay_b = to_blocks(decay_logarithm)
    beta_b = to_blocks(beta)
    cumulative = jnp.cumsum(decay_b, axis=-1)
    positions = jnp.arange(BLOCK)
    causal = positions[:, None] >= positions[None, :]
    strict = positions[:, None] > positions[None, :]
    spread = cumulative[..., :, None] - cumulative[..., None, :]
    weights = jnp.where(causal, jnp.exp(jnp.where(causal, spread, 0.0)), 0.0)
    keys_beta = keys_b * beta_b[..., None]
    values_beta = values_b * beta_b[..., None]
    intersection = jnp.einsum('nhid,nhjd->nhij', keys_beta, keys_b, precision=lax.Precision.HIGHEST)
    lower_part = jnp.where(strict, intersection * weights, 0.0) + jnp.eye(BLOCK, dtype=jnp.float32)
    right_side = jnp.concatenate([values_beta, keys_beta * jnp.exp(cumulative)[..., None]], axis=-1)
    solved = jax.scipy.linalg.solve_triangular(lower_part, right_side, lower=True, unit_diagonal=True)
    value_depth = values.shape[-1]
    update = solved[..., :value_depth]
    project = solved[..., value_depth:]
    scores = jnp.einsum('nhid,nhjd->nhij', query_b, keys_b, precision=lax.Precision.HIGHEST) * weights
    query_dec = query_b * jnp.exp(cumulative)[..., None]
    keys_dec = keys_b * jnp.exp(cumulative[..., -1:] - cumulative)[..., None]
    carry_decay = jnp.exp(cumulative[..., -1])
    return (scores, query_dec, keys_dec, update, project, carry_decay)

def run_blocks(state, terms):

    def advance(carried, inputs):
        scores, query_dec, keys_dec, update, project, carry_decay = inputs
        fresh = update - jnp.einsum('hcd,hde->hce', project, carried, precision=lax.Precision.HIGHEST)
        output = jnp.einsum('hcd,hde->hce', query_dec, carried, precision=lax.Precision.HIGHEST)
        output = output + jnp.einsum('hij,hje->hie', scores, fresh, precision=lax.Precision.HIGHEST)
        carried = carried * carry_decay[:, None, None] + jnp.einsum('hcd,hce->hde', keys_dec, fresh, precision=lax.Precision.HIGHEST)
        return (carried, output)
    final_state, outputs = lax.scan(advance, state, terms)
    return outputs

def reference(tokens, input_norm_scale, mean_input_weight, query_matrix, key_matrix, value_matrix, strength_weight, decay_input_weight, causal_filter_weight, head_decay_logrates, decay_input_shift, strength_shift, decay_spike, head_norm_scale, group_mixing_weight, mean_channel_scale, mean_output_weight, delta_output_weight):
    normed = scale_rows(tokens.astype(jnp.float32), input_norm_scale).astype(jnp.bfloat16)
    pool_raw = jnp.dot(normed.astype(jnp.float32), mean_input_weight.astype(jnp.float32), preferred_element_type=jnp.float32).astype(jnp.bfloat16)
    query_raw = jnp.dot(normed.astype(jnp.float32), query_matrix.astype(jnp.float32), preferred_element_type=jnp.float32).astype(jnp.bfloat16)
    key_raw = jnp.dot(normed.astype(jnp.float32), key_matrix.astype(jnp.float32), preferred_element_type=jnp.float32).astype(jnp.bfloat16)
    value_raw = jnp.dot(normed.astype(jnp.float32), value_matrix.astype(jnp.float32), preferred_element_type=jnp.float32).astype(jnp.bfloat16)
    beta_raw = jnp.dot(normed.astype(jnp.float32), strength_weight.astype(jnp.float32), preferred_element_type=jnp.float32).astype(jnp.bfloat16)
    decay_unshaped = jnp.dot(normed.astype(jnp.float32), decay_input_weight.astype(jnp.float32), preferred_element_type=jnp.float32).astype(jnp.bfloat16)
    qkv_raw = jnp.concatenate([query_raw, key_raw, value_raw], axis=1)
    extended_qkv = jnp.concatenate([jnp.zeros((CONV - 1, 3 * GDN_W), jnp.bfloat16), qkv_raw], axis=0).astype(jnp.float32)
    convolved = causal_taps(extended_qkv, causal_filter_weight.reshape(CONV, 3 * GDN_W).astype(jnp.float32), SEQUENCE_TOKENS)
    query = unit_rows(convolved[:, :GDN_W].reshape(SEQUENCE_TOKENS, MIXER_HEADS, HEAD_DIM)) * HEAD_DIM ** (-0.5)
    keys = unit_rows(convolved[:, GDN_W:2 * GDN_W].reshape(SEQUENCE_TOKENS, MIXER_HEADS, HEAD_DIM))
    values = convolved[:, 2 * GDN_W:].reshape(SEQUENCE_TOKENS, MIXER_HEADS, HEAD_DIM)
    beta = jax.nn.sigmoid(beta_raw.astype(jnp.float32) + strength_shift)
    decay_logarithm = -jnp.exp(head_decay_logrates) * jax.nn.softplus(decay_unshaped.astype(jnp.float32) + decay_input_shift) + decay_spike
    terms = block_terms(query, keys, values, decay_logarithm, beta)
    outputs = run_blocks(jnp.zeros((MIXER_HEADS, HEAD_DIM, HEAD_DIM), jnp.float32), terms)
    delta_rows = jnp.swapaxes(outputs, 1, 2).reshape(SEQUENCE_TOKENS, MIXER_HEADS, HEAD_DIM)
    delta_mixed = scale_rows(delta_rows, head_norm_scale).astype(jnp.bfloat16).reshape(SEQUENCE_TOKENS, GDN_W)
    group_ids = (jnp.arange(POOL_W) // GROUP_DIM).astype(jnp.int32)
    positions = jnp.arange(SEQUENCE_TOKENS).astype(jnp.int32)
    pool_diff = pool_means(jnp.zeros((15, POOL_W), jnp.bfloat16), pool_raw, group_ids, positions)
    pooled = jnp.einsum('tgc,gcd->tgd', pool_diff.astype(jnp.float32).reshape(SEQUENCE_TOKENS, POOL_GROUPS, GROUP_DIM), group_mixing_weight.astype(jnp.float32))
    pool_mixed = (pooled.reshape(SEQUENCE_TOKENS, POOL_W) * mean_channel_scale.astype(jnp.float32)).astype(jnp.bfloat16)
    pool_slice = POOL_W // N_TP
    delta_slice = GDN_W // N_TP
    summed = jnp.zeros((SEQUENCE_TOKENS, D), jnp.float32)
    for shard_index in range(N_TP):
        pool_part = pool_mixed[:, shard_index * pool_slice:(shard_index + 1) * pool_slice]
        delta_part = delta_mixed[:, shard_index * delta_slice:(shard_index + 1) * delta_slice]
        rows_in = jnp.concatenate([pool_part, delta_part], axis=1)
        weight_rows = jnp.concatenate([mean_output_weight[shard_index * pool_slice:(shard_index + 1) * pool_slice], delta_output_weight[shard_index * delta_slice:(shard_index + 1) * delta_slice]], axis=0)
        partial_sum = jnp.dot(rows_in.astype(jnp.float32), weight_rows.astype(jnp.float32), preferred_element_type=jnp.float32).astype(jnp.bfloat16)
        summed = summed + partial_sum.astype(jnp.float32)
    return summed.astype(jnp.bfloat16)
```

```python
import jax
import jax.numpy as jnp
from jax import lax
from jax.experimental import pallas as pl
from jax.experimental.pallas import tpu as pltpu
from jax.sharding import PartitionSpec as P

GROUP_DIM = 128
HEAD_DIM = 128
CONV = 4
BLOCK = 64


EPSILON = 1e-06


def shifted_2(block, axis, distance):
    devices = range(lax.axis_size(axis))
    route = [(i - distance, i) for i in devices if i - distance in devices]
    return lax.ppermute(block, axis, route)


def scale_rows(values, gain_vec):
    squares = jnp.mean(values * values, axis=-1, keepdims=True)
    return values * lax.rsqrt(squares + EPSILON) * gain_vec.astype(jnp.float32)


def pool_means(previous, current, group_ids, positions):
    pool_reach = 15
    rows_out = current.shape[0]
    extended = jnp.concatenate([previous, current], axis=0).astype(jnp.float32)
    window_size = jnp.left_shift(jnp.int32(2), group_ids % 4)
    windowed = jnp.zeros(current.shape, jnp.float32)
    for lag_rows in range(pool_reach + 1):
        shifted = extended[pool_reach - lag_rows : pool_reach - lag_rows + rows_out]
        windowed = windowed + jnp.where(lag_rows < window_size[None, :], shifted, 0.0)
    counts = jnp.minimum(positions[:, None] + 1, window_size[None, :]).astype(jnp.float32)
    return (windowed / counts - extended[pool_reach:]).astype(jnp.bfloat16)


BF16 = jnp.bfloat16
F32 = jnp.float32
HALO = 8


def dot(left, right):
    return jnp.dot(left.astype(BF16), right.astype(BF16), preferred_element_type=F32)


def dot_nt(left, right):
    return lax.dot_general(
        left.astype(BF16),
        right.astype(BF16),
        (((1,), (1,)), ((), ())),
        preferred_element_type=F32,
    )


def dot_tn(left, right):
    return lax.dot_general(
        left.astype(BF16),
        right.astype(BF16),
        (((0,), (0,)), ((), ())),
        preferred_element_type=F32,
    )


def unit_rows(values):
    return values * lax.rsqrt(jnp.sum(values * values, axis=-1, keepdims=True) + EPSILON)


def delta_kernel(heads, depth, chunk, *refs):
    (q_ref, k_ref, v_ref, hq_ref, hk_ref, hv_ref, tap_ref, beta_ref, decay_ref) = refs[:9]
    out_ref, eff_ref, state_ref, carry, halo = refs[9:]
    step = pl.program_id(0)
    width = heads * depth
    row = lax.broadcasted_iota(jnp.int32, (chunk, chunk), 0)
    col = lax.broadcasted_iota(jnp.int32, (chunk, chunk), 1)
    causal = row >= col
    strict = row > col
    eye = jnp.where(row == col, 1.0, 0.0)
    lane = lax.broadcasted_iota(jnp.int32, (depth, 2 * depth), 1)
    sub = lax.broadcasted_iota(jnp.int32, (depth, 2 * depth), 0)

    @pl.when(step == 0)
    def _():
        for h in range(heads):
            carry[h] = jnp.where(lane == sub + depth, 1.0, 0.0)
        halo[0] = hq_ref[...].astype(F32)
        halo[1] = hk_ref[...].astype(F32)
        halo[2] = hv_ref[...].astype(F32)

    convolved = []
    for r, ref in enumerate((q_ref, k_ref, v_ref)):
        current = ref[...].astype(F32)
        extended = jnp.concatenate([halo[r], current], axis=0)
        halo[r] = current[chunk - HALO :]
        total = jnp.zeros((chunk, width), F32)
        for i in range(CONV):
            start = HALO - (CONV - 1) + i
            taps = tap_ref[i, r : r + 1, :].astype(F32)
            total = total + taps * extended[start : start + chunk]
        convolved.append(total / (1.0 + jnp.exp(-total)))
    tri = jnp.where(causal, 1.0, 0.0)
    decay = decay_ref[...]
    cum_cols = jnp.dot(tri, decay, preferred_element_type=F32, precision=lax.Precision.HIGHEST)
    cum_rows = lax.dot_general(
        decay,
        tri,
        (((0,), (1,)), ((), ())),
        preferred_element_type=F32,
        precision=lax.Precision.HIGHEST,
    )
    base = min(16, chunk)
    hs = range(heads)
    q = [unit_rows(convolved[0][:, h * depth : (h + 1) * depth]) * depth ** (-0.5) for h in hs]
    k = [unit_rows(convolved[1][:, h * depth : (h + 1) * depth]) for h in hs]
    v = [convolved[2][:, h * depth : (h + 1) * depth] for h in hs]
    cum = [cum_cols[:, h : h + 1] for h in hs]
    last = [cum_cols[chunk - 1 : chunk, h : h + 1] for h in hs]
    beta = [beta_ref[:, h : h + 1] for h in hs]
    weights = [
        jnp.where(causal, jnp.exp(jnp.where(causal, cum[h] - cum_rows[h : h + 1, :], 0.0)), 0.0)
        for h in hs
    ]
    kb = [k[h] * beta[h] for h in hs]
    lower = [jnp.where(strict, dot_nt(kb[h], k[h]) * weights[h], 0.0) for h in hs]
    power = [jnp.where(row // base == col // base, lower[h], 0.0) for h in hs]
    inverse = [eye - power[h] for h in hs]
    reach = 2
    while reach < base:
        power = [dot(power[h], power[h]) for h in hs]
        inverse = [inverse[h] + dot(inverse[h], power[h]) for h in hs]
        reach *= 2
    size = base
    while size < chunk:
        pair = (row // (2 * size) == col // (2 * size)) & (row // size != col // size)
        right = [dot(jnp.where(pair, lower[h], 0.0), inverse[h]) for h in hs]
        inverse = [inverse[h] - dot(inverse[h], right[h]) for h in hs]
        size *= 2
    grow = [jnp.exp(cum[h]) for h in hs]
    sides = [jnp.concatenate([v[h] * beta[h], kb[h] * grow[h]], axis=1) for h in hs]
    solved = [dot(inverse[h], sides[h]) for h in hs]
    scores = [dot_nt(q[h], k[h]) * weights[h] for h in hs]
    kd = [k[h] * jnp.exp(last[h] - cum[h]) for h in hs]
    zeros = jnp.zeros((chunk, depth), F32)
    state = [carry[h] for h in hs]
    fresh = [
        jnp.concatenate([solved[h][:, :depth], zeros], axis=1) - dot(solved[h][:, depth:], state[h])
        for h in hs
    ]
    outs = [dot(q[h] * grow[h], state[h]) + dot(scores[h], fresh[h]) for h in hs]
    for h in hs:
        carry[h] = state[h] * jnp.exp(last[h]) + dot_tn(kd[h], fresh[h])
        out_ref[:, h * depth : (h + 1) * depth] = outs[h][:, :depth]
        eff_ref[:, h * depth : (h + 1) * depth] = outs[h][:, depth:].astype(BF16)
        state_ref[h] = carry[h]


def delta_pass(q, k, v, hq, hk, hv, taps, beta, decay, depth):
    rows, width = q.shape
    heads = beta.shape[1]
    chunk = min(128, rows)
    whole = lambda shape: pl.BlockSpec(shape, lambda i: (0,) * len(shape))
    tile = pl.BlockSpec((chunk, width), lambda i: (i, 0))
    slim = pl.BlockSpec((chunk, heads), lambda i: (i, 0))
    return pl.pallas_call(
        lambda *refs: delta_kernel(heads, depth, chunk, *refs),
        grid=(rows // chunk,),
        in_specs=[tile] * 3 + [whole(hq.shape)] * 3 + [whole(taps.shape), slim, slim],
        out_specs=[tile, tile, whole((heads, depth, 2 * depth))],
        out_shape=[
            jax.ShapeDtypeStruct((rows, width), F32),
            jax.ShapeDtypeStruct((rows, width), BF16),
            jax.ShapeDtypeStruct((heads, depth, 2 * depth), F32),
        ],
        scratch_shapes=[
            pltpu.VMEM((heads, depth, 2 * depth), F32),
            pltpu.VMEM((3, HALO, width), F32),
        ],
        compiler_params=pltpu.CompilerParams(
            dimension_semantics=("arbitrary",), vmem_limit_bytes=32 * 1024 * 1024
        ),
        cost_estimate=pl.CostEstimate(
            flops=rows * width * 4096, bytes_accessed=rows * width * 12, transcendentals=0
        ),
    )(q, k, v, hq, hk, hv, taps, beta, decay)


def finish_kernel(heads, depth, out_ref, eff_ref, state_ref, gain_ref, mixed_ref):
    gain = gain_ref[...].astype(F32)
    for h in range(heads):
        cols = slice(h * depth, (h + 1) * depth)
        raw = out_ref[:, cols] + dot(eff_ref[:, cols], state_ref[h])
        scale = lax.rsqrt(jnp.mean(raw * raw, axis=-1, keepdims=True) + EPSILON)
        mixed_ref[:, cols] = (raw * scale * gain).astype(BF16)


def finish_pass(out, eff, incoming, gain):
    rows, width = out.shape
    heads, depth = incoming.shape[:2]
    chunk = min(256, rows)
    tile = pl.BlockSpec((chunk, width), lambda i: (i, 0))
    return pl.pallas_call(
        lambda *refs: finish_kernel(heads, depth, *refs),
        grid=(rows // chunk,),
        in_specs=[
            tile,
            tile,
            pl.BlockSpec(incoming.shape, lambda i: (0, 0, 0)),
            pl.BlockSpec((1, depth), lambda i: (0, 0)),
        ],
        out_specs=tile,
        out_shape=jax.ShapeDtypeStruct((rows, width), BF16),
        compiler_params=pltpu.CompilerParams(dimension_semantics=("arbitrary",)),
    )(out, eff, incoming, gain.reshape(1, depth))


def earlier_state(state, depth):
    def compose(later, earlier):
        pushed = jnp.einsum(
            "hde,hef->hdf", later[..., depth:].astype(BF16), earlier, preferred_element_type=F32
        )
        own = jnp.concatenate([later[..., :depth], jnp.zeros_like(later[..., depth:])], axis=-1)
        return own + pushed

    held = shifted_2(state.astype(BF16), "sp", 1)
    count = lax.axis_size("sp")
    distance = 1
    while distance < count - 1:
        sent = held if 2 * distance < count - 1 else held[..., :depth]
        arrived = shifted_2(sent, "sp", distance)
        if 2 * distance < count - 1:
            held = compose(held.astype(F32), arrived).astype(BF16)
        else:
            held = held[..., :depth].astype(F32) + jnp.einsum(
                "hde,hef->hdf", held[..., depth:], arrived, preferred_element_type=F32
            )
        distance *= 2
    return held[..., :depth].astype(BF16)


def per_device(
    tokens,
    input_norm_scale,
    mean_input_weight,
    query_matrix,
    key_matrix,
    value_matrix,
    strength_weight,
    decay_input_weight,
    causal_filter_weight,
    head_decay_logrates,
    decay_input_shift,
    strength_shift,
    decay_spike,
    head_norm_scale,
    group_mixing_weight,
    mean_channel_scale,
    mean_output_weight,
    delta_output_weight,
):
    tok_rows = tokens.shape[0]
    pool_cols = mean_input_weight.shape[1]
    delta_cols = query_matrix.shape[1]
    head_count = strength_weight.shape[1]
    head_depth = delta_cols // head_count
    groups_dev = pool_cols // GROUP_DIM
    tp_index = lax.axis_index("tp")
    sp_index = lax.axis_index("sp")
    normed = scale_rows(tokens.astype(jnp.float32), input_norm_scale).astype(jnp.bfloat16)
    narrow = lax.all_gather(
        jnp.concatenate([strength_weight, decay_input_weight], axis=1), "sp", axis=0, tiled=True
    )
    project = lambda weight: jnp.dot(normed, weight, preferred_element_type=F32).astype(BF16)
    gather = lambda weight: lax.all_gather(weight, "sp", axis=0, tiled=True)
    key_raw = project(gather(key_matrix))
    query_raw = project(gather(query_matrix))
    value_raw = project(gather(value_matrix))
    pool_raw = project(gather(mean_input_weight))
    narrow_raw = project(narrow)
    beta_raw = narrow_raw[:, :head_count]
    decay_unshaped = narrow_raw[:, head_count:]
    pool_reach = 15
    halos = shifted_2(
        tuple(raw[tok_rows - HALO :] for raw in (query_raw, key_raw, value_raw)), "sp", 1
    )
    previous_pool = shifted_2(pool_raw[tok_rows - pool_reach :], "sp", 1)
    taps = lax.dynamic_slice_in_dim(causal_filter_weight, tp_index * delta_cols, delta_cols, 2)
    rate_logarithm = lax.dynamic_slice_in_dim(
        head_decay_logrates, tp_index * head_count, head_count
    )
    shift_amounts = lax.dynamic_slice_in_dim(decay_input_shift, tp_index * head_count, head_count)
    strength_offsets = lax.dynamic_slice_in_dim(strength_shift, tp_index * head_count, head_count)
    beta = jax.nn.sigmoid(beta_raw.astype(jnp.float32) + strength_offsets)
    decay_logarithm = (
        -jnp.exp(rate_logarithm)
        * jax.nn.softplus(decay_unshaped.astype(jnp.float32) + shift_amounts)
        + decay_spike
    )
    out_local, out_reach, state = delta_pass(
        query_raw, key_raw, value_raw, *halos, taps, beta, decay_logarithm, head_depth
    )
    incoming = earlier_state(state, head_depth)
    delta_mixed = finish_pass(out_local, out_reach, incoming, head_norm_scale)
    group_ids = tp_index * groups_dev + jnp.arange(pool_cols) // GROUP_DIM
    positions = sp_index * tok_rows + jnp.arange(tok_rows)
    pool_diff = pool_means(previous_pool, pool_raw, group_ids, positions)
    local_mix = lax.dynamic_slice_in_dim(group_mixing_weight, tp_index * groups_dev, groups_dev, 0)
    pooled = jnp.einsum(
        "tgc,gcd->tgd",
        pool_diff.reshape(tok_rows, groups_dev, GROUP_DIM),
        local_mix,
        preferred_element_type=jnp.float32,
    )
    pool_scale = lax.dynamic_slice_in_dim(mean_channel_scale, tp_index * pool_cols, pool_cols)
    pool_mixed = (pooled.reshape(tok_rows, pool_cols) * pool_scale.astype(jnp.float32)).astype(
        jnp.bfloat16
    )
    mixed = jnp.concatenate([pool_mixed, delta_mixed], axis=1)
    pool_weight_rows, delta_weight_rows = (
        lax.all_gather(mean_output_weight, "sp", axis=1, tiled=True),
        lax.all_gather(delta_output_weight, "sp", axis=1, tiled=True),
    )
    out_weight = jnp.concatenate([pool_weight_rows, delta_weight_rows], axis=0)
    return lax.psum_scatter(
        jnp.dot(mixed, out_weight, preferred_element_type=jnp.float32).astype(jnp.bfloat16),
        "tp",
        scatter_dimension=0,
        tiled=True,
    )


def solution(mesh):
    return jax.shard_map(
        per_device,
        mesh=mesh,
        in_specs=(
            P("sp", None),
            P(),
            P("sp", "tp"),
            P("sp", "tp"),
            P("sp", "tp"),
            P("sp", "tp"),
            P("sp", "tp"),
            P("sp", "tp"),
            P(),
            P(),
            P(),
            P(),
            P("sp", "tp"),
            P(),
            P(),
            P(),
            P("tp", "sp"),
            P("tp", "sp"),
        ),
        out_specs=P(("sp", "tp"), None),
        check_vma=False,
    )
```
